256 devices in a mesh: kv: 32 (over z, y), tp: 8 (over x, core).
Axes of the slice: x: 4, y: 4, z: 8, core: 2. Of those that a mesh axis runs over, the one named last changes fastest.
Arguments:
- tokens: bfloat16 [128, 4096], P(None, 'kv'), may hold values from -8 to 8, as said below
- attn_gain: float32 [4096], P('kv'), may hold values from 0.1 to 1.9
- query_weight: bfloat16 [4096, 1024], P('kv', 'tp'), may hold values from -0.09375 to 0.09375
- key_weight: bfloat16 [4096, 1024], P('kv', 'tp'), may hold values from -0.09375 to 0.09375
- value_weight: bfloat16 [4096, 2048], P('kv', 'tp'), may hold values from -0.09375 to 0.09375
- outgate_weight: bfloat16 [4096, 2048], P('kv', 'tp'), may hold values from -0.09375 to 0.09375
- code_weight: bfloat16 [4096, 16], P('kv'), may hold values from -0.09375 to 0.09375
- decay_weight: bfloat16 [16, 1024], P(None, 'tp'), may hold values from -6 to 6
- decay_bias: float32 [1024], P('tp'), may hold values from -4 to 2
- head_gain: float32 [256], replicated, may hold values from 0.1 to 1.9
- key_cache: bfloat16 [128, 64, 8, 128], P('kv', None, 'tp'), may hold values from -6 to 6
- value_cache: bfloat16 [128, 64, 8, 256], P('kv', None, 'tp'), may hold values from -6 to 6
- decay_cache: float32 [128, 64, 8, 128], P('kv', None, 'tp'), may hold values from -1.1 to 0
- carried_state: float32 [128, 8, 128, 256], P('kv', 'tp'), may hold values from -24 to 24
- lengths: int32 [128], P('kv'), may hold values from 1 to 64, 3328 in all
- output_weight: bfloat16 [2048, 4096], P('tp', 'kv'), may hold values from -0.125 to 0.125
- mlp_gain: float32 [4096], P('kv'), may hold values from 0.1 to 1.9
- gate_weight: bfloat16 [4096, 11008], P('kv', 'tp'), may hold values from -0.09375 to 0.09375
- up_weight: bfloat16 [4096, 11008], P('kv', 'tp'), may hold values from -0.09375 to 0.09375
- down_weight: bfloat16 [11008, 4096], P('tp', 'kv'), may hold values from -0.0546875 to 0.0546875
Outputs:
- layer_out: bfloat16 [128, 4096], P(None, 'kv')
- new_keys: bfloat16 [128, 8, 128], P('kv', 'tp')
- new_values: bfloat16 [128, 8, 256], P('kv', 'tp')
The draws below stay inside these ranges and needn't reach their ends.
Inputs may be any that keep to these rules, and one draw needn't show every extreme that they name: `tokens`: the features of a row have unlike scales. Sequence b's new token comes right after its lengths[b] live positions; positions from lengths[b] on take no part.
All inputs are finite; a program needn't handle non-finite values. No bound on the sum of `lengths` on one device may be relied on, other than what follows from the above.
Results may differ from the reference program's by a relative error of at most 0.025.
Values may be sent and summed in bfloat16 or wider, within the bound.
A program may use at most 64 MiB of HBM per device.

```python
import math
import jax
import jax.numpy as jnp
import numpy as np
from jax import lax

WIDTH = 4096
HEAD_COUNT = 8
KEY_DIM = 128
VALUE_DIM = 256
KEY_WIDTH = 1024
VALUE_WIDTH = 2048
GATE_RANK = 16
MLP_WIDTH = 11008
BLOCK_SPAN = 64
BATCH_TOTAL = 128
N_TP = 8


def draw_tokens(key, part):
    base_key, rough_key = jax.random.split(jax.random.fold_in(key, 11), 2)
    column = jnp.arange(WIDTH, dtype=jnp.float32) / WIDTH
    jaggedness = jax.random.uniform(rough_key, (WIDTH,), jnp.float32, 0.5, 2.0)
    scales = 10.0 ** (column - 0.75) * jaggedness
    values = jax.random.normal(base_key, (BATCH_TOTAL, WIDTH), jnp.float32) * scales[None, :]
    return jnp.clip(values, -8.0, 8.0).astype(jnp.bfloat16)


def draw_decay_cache(key, part):
    random_split_keys = jax.random.split(jax.random.fold_in(key, 23), 5)
    slowest = 0.002
    fastest = 0.12
    channel_frequencies = jnp.exp(jax.random.uniform(random_split_keys[0], (1, 1, HEAD_COUNT, KEY_DIM), jnp.float32, math.log(slowest), math.log(fastest)))
    sequence_wise = jnp.exp(jax.random.uniform(random_split_keys[1], (BATCH_TOTAL, 1, 1, 1), jnp.float32, math.log(0.5), math.log(2.0)))
    jaggedness = jax.random.uniform(random_split_keys[2], (BATCH_TOTAL, BLOCK_SPAN, HEAD_COUNT, KEY_DIM), jnp.float32, 0.5, 1.5)
    spike_events = jax.random.randint(random_split_keys[3], (BATCH_TOTAL, BLOCK_SPAN, 1, 1), 0, BLOCK_SPAN) < 3
    spike_removal = jax.random.uniform(random_split_keys[4], (BATCH_TOTAL, BLOCK_SPAN, HEAD_COUNT, 1), jnp.float32, math.log(0.5), math.log(0.8))
    return -channel_frequencies * sequence_wise * jaggedness + jnp.where(spike_events, spike_removal, 0.0)


def levels(stream_key, extent, shards, smallest, top_value):
    def one(dim, blocks):
        heights = jax.random.uniform(jax.random.fold_in(jax.random.fold_in(stream_key, 6), dim), (blocks,), jnp.float32, smallest / len(shards), top_value / len(shards))
        return jnp.repeat(jnp.exp(heights), extent[dim] // blocks).reshape((-1,) + (1,) * (len(extent) - dim - 1))

    level = one(*shards[0])
    for cut in shards[1:]:
        level = level * one(*cut)
    return level


def split_up(amount, total, limit, slope):
    loads = [(1 << 20) // math.isqrt(grade ** slope) + 1 for grade in range(2, amount + 1)]
    surplus, given = total - limit - (amount - 1), [1] * (amount - 1)
    while surplus > 0:
        candidates = [i for i in range(amount - 1) if given[i] < limit]
        whole, remaining = sum([loads[i] for i in candidates]), surplus
        for i in candidates:
            more = min(limit - given[i], max(1, remaining * loads[i] // whole), surplus)
            given[i] = given[i] + more
            surplus = surplus - more
    return np.array([limit] + given)


def ragged_sizes(own_key, count, total, limit, slope):
    if count == 2:
        one = jax.random.randint(own_key, (), max(1, total - limit), min(limit, total - 1) + 1)
        return jnp.stack([one, total - one])
    sizes = jnp.asarray(split_up(count, total, limit, slope), jnp.int32)
    couples = (count - 1) // 2
    source_of, taker = sizes[1:1 + 2 * couples:2], sizes[2:2 + 2 * couples:2]
    room = jnp.minimum(source_of - 1, limit - taker)
    shifted = jax.random.randint(jax.random.fold_in(own_key, 1), (couples,), 0, 1 << 20) % (room + 1)
    sizes = sizes.at[1:1 + 2 * couples:2].set(source_of - shifted).at[2:2 + 2 * couples:2].set(taker + shifted)
    return sizes[jax.random.permutation(jax.random.fold_in(own_key, 2), count)]


def scatter_about(own_key, dims, scale, most, pieces=(), kind=jnp.bfloat16):
    result = jax.random.normal(own_key, dims, jnp.float32) * scale
    if len(pieces) > 0:
        result = levels(own_key, dims, pieces, -0.22, 0.18) * result
    return jnp.clip(result, min=-most, max=most).astype(kind)


def setup_inputs(seed: int = 0) -> dict:
    streams_of = jax.random.split(jax.random.key(seed), 21)
    return {
        "tokens": draw_tokens(jax.random.fold_in(streams_of[20], 71), 0),
        "attn_gain": jnp.clip(1.0 + 0.18 * jax.random.normal(streams_of[1], (WIDTH,), jnp.float32), 0.1, 1.9),
        "query_weight": scatter_about(streams_of[2], (WIDTH, KEY_WIDTH), WIDTH ** -0.5, 0.09375, ((0, 32), (1, 8))),
        "key_weight": scatter_about(streams_of[3], (WIDTH, KEY_WIDTH), WIDTH ** -0.5, 0.09375, ((0, 32), (1, 8))),
        "value_weight": scatter_about(streams_of[4], (WIDTH, VALUE_WIDTH), WIDTH ** -0.5, 0.09375, ((0, 32), (1, 8))),
        "outgate_weight": scatter_about(streams_of[5], (WIDTH, VALUE_WIDTH), WIDTH ** -0.5, 0.09375, ((0, 32), (1, 8))),
        "code_weight": scatter_about(streams_of[6], (WIDTH, GATE_RANK), WIDTH ** -0.5, 0.09375, ((0, 32),)),
        "decay_weight": scatter_about(streams_of[7], (GATE_RANK, KEY_WIDTH), 1 ** -0.5, 6.0, ((1, 8),)),
        "decay_bias": jnp.clip(-4.0 + 6.0 * jax.random.uniform(streams_of[8], (KEY_WIDTH,), jnp.float32) ** levels(streams_of[8], (KEY_WIDTH,), ((0, 8),), -0.2, 0.2), -4.0, 2.0),
        "head_gain": jnp.clip(1.0 + 0.18 * jax.random.normal(streams_of[9], (VALUE_DIM,), jnp.float32), 0.1, 1.9),
        "key_cache": scatter_about(streams_of[10], (BATCH_TOTAL, BLOCK_SPAN, HEAD_COUNT, KEY_DIM), 1.0, 6.0, ((0, 32), (2, 8))),
        "value_cache": scatter_about(streams_of[11], (BATCH_TOTAL, BLOCK_SPAN, HEAD_COUNT, VALUE_DIM), 1.0, 6.0, ((0, 32), (2, 8))),
        "decay_cache": draw_decay_cache(jax.random.fold_in(streams_of[20], 71), 0),
        "carried_state": scatter_about(streams_of[13], (BATCH_TOTAL, HEAD_COUNT, KEY_DIM, VALUE_DIM), 4.0, 24.0, ((0, 32), (1, 8)), jnp.float32),
        "lengths": ragged_sizes(streams_of[14], BATCH_TOTAL, BATCH_TOTAL * (13 * BLOCK_SPAN // 32), BLOCK_SPAN, 2).astype(jnp.int32),
        "output_weight": scatter_about(streams_of[15], (VALUE_WIDTH, WIDTH), VALUE_WIDTH ** -0.5, 0.125, ((0, 8), (1, 32))),
        "mlp_gain": jnp.clip(1.0 + 0.18 * jax.random.normal(streams_of[16], (WIDTH,), jnp.float32), 0.1, 1.9),
        "gate_weight": scatter_about(streams_of[17], (WIDTH, MLP_WIDTH), WIDTH ** -0.5, 0.09375, ((0, 32), (1, 8))),
        "up_weight": scatter_about(streams_of[18], (WIDTH, MLP_WIDTH), WIDTH ** -0.5, 0.09375, ((0, 32), (1, 8))),
        "down_weight": scatter_about(streams_of[19], (MLP_WIDTH, WIDTH), MLP_WIDTH ** -0.5, 0.0546875, ((0, 8), (1, 32))),
    }


EPS = 1e-06
GATE_TEMP = 16.0

def block_attention(queries, new_keys, new_values, new_decay, key_cache, value_cache, decay_cache, carried_state, lengths):
    positions = jnp.arange(key_cache.shape[1], dtype=jnp.int32)
    live_mask = positions[None, :] < lengths[:, None]
    kept_decay = jnp.where(live_mask[:, :, None, None], decay_cache, jnp.zeros_like(decay_cache))
    later_sum = lax.cumsum(kept_decay, axis=1, reverse=True) - kept_decay
    total_decay = lax.optimization_barrier(jnp.sum(kept_decay, axis=1))
    decayed = queries.astype(jnp.float32) * jnp.exp(new_decay)
    carried = jnp.einsum('bhd,bhde->bhe', decayed * jnp.exp(total_decay), carried_state, precision=lax.Precision.HIGHEST)
    keyed_cache = key_cache.astype(jnp.float32) * jnp.exp(later_sum)
    scores = jnp.einsum('bhd,bshd->bhs', decayed, keyed_cache, precision=lax.Precision.HIGHEST)
    scores = jnp.where(live_mask[:, None, :], scores, jnp.zeros_like(scores)).astype(jnp.bfloat16)
    within = jnp.einsum('bhs,bshe->bhe', scores.astype(jnp.float32), value_cache.astype(jnp.float32))
    own_score = lax.optimization_barrier(jnp.sum(queries.astype(jnp.float32) * new_keys.astype(jnp.float32), axis=-1))
    return carried + within + own_score[..., None] * new_values.astype(jnp.float32)

def summed_by_group(left, weight, groups):
    row_count, inner_dim = left.shape
    group_parts = jnp.einsum('bni,nid->bnd', left.reshape(row_count, groups, inner_dim // groups).astype(jnp.float32), weight.reshape(groups, inner_dim // groups, weight.shape[1]).astype(jnp.float32))
    group_parts = lax.optimization_barrier(group_parts.astype(jnp.bfloat16))
    return lax.optimization_barrier(jnp.sum(group_parts.astype(jnp.float32), axis=1))

def reference(tokens, attn_gain, query_weight, key_weight, value_weight, outgate_weight, code_weight, decay_weight, decay_bias, head_gain, key_cache, value_cache, decay_cache, carried_state, lengths, output_weight, mlp_gain, gate_weight, up_weight, down_weight):
    token_f = tokens.astype(jnp.float32)
    scaled = (token_f * attn_gain[None, :]).astype(jnp.bfloat16)
    inv_rms = lax.rsqrt(lax.optimization_barrier(jnp.mean(token_f * token_f, axis=1, keepdims=True)) + EPS)

    def project(weight):
        return jnp.dot(scaled, weight, preferred_element_type=jnp.float32) * inv_rms
    queries = (project(query_weight) * KEY_DIM ** (-0.5)).astype(jnp.bfloat16).reshape(BATCH_TOTAL, HEAD_COUNT, KEY_DIM)
    new_keys = project(key_weight).astype(jnp.bfloat16).reshape(BATCH_TOTAL, HEAD_COUNT, KEY_DIM)
    new_values = project(value_weight).astype(jnp.bfloat16).reshape(BATCH_TOTAL, HEAD_COUNT, VALUE_DIM)
    out_gate = project(outgate_weight).astype(jnp.bfloat16).reshape(BATCH_TOTAL, HEAD_COUNT, VALUE_DIM)
    gate_code = project(code_weight).astype(jnp.bfloat16)
    pre_gate = jnp.dot(gate_code, decay_weight, preferred_element_type=jnp.float32) + decay_bias[None, :]
    new_decay = (jax.nn.log_sigmoid(pre_gate) / GATE_TEMP).reshape(BATCH_TOTAL, HEAD_COUNT, KEY_DIM)
    mixed_heads = block_attention(queries, new_keys, new_values, new_decay, key_cache, value_cache, decay_cache, carried_state, lengths)
    normed = mixed_heads * lax.rsqrt(lax.optimization_barrier(jnp.mean(mixed_heads * mixed_heads, axis=-1, keepdims=True)) + EPS) * head_gain
    heads_out = (normed * jax.nn.silu(out_gate.astype(jnp.float32))).astype(jnp.bfloat16).reshape(BATCH_TOTAL, HEAD_COUNT * VALUE_DIM)
    attended = summed_by_group(heads_out, output_weight, N_TP)
    middle = (token_f + attended).astype(jnp.bfloat16)
    mid_f = middle.astype(jnp.float32)
    scaled_mid = (mid_f * mlp_gain[None, :]).astype(jnp.bfloat16)
    inv_mid = lax.rsqrt(lax.optimization_barrier(jnp.mean(mid_f * mid_f, axis=1, keepdims=True)) + EPS)
    gate_act = jnp.dot(scaled_mid, gate_weight, preferred_element_type=jnp.float32) * inv_mid
    up_act = jnp.dot(scaled_mid, up_weight, preferred_element_type=jnp.float32) * inv_mid
    hidden = (jax.nn.silu(gate_act) * up_act).astype(jnp.bfloat16)
    lifted = summed_by_group(hidden, down_weight, N_TP)
    layer_out = (mid_f + lifted).astype(jnp.bfloat16)
    return (layer_out, new_keys, new_values)
```

```python
import functools

import jax
import jax.numpy as jnp
from jax import lax
from jax.experimental import pallas as pl
from jax.experimental.pallas import tpu as pltpu
from jax.sharding import PartitionSpec as P

MESH = pl.DeviceIdType.MESH
F32 = jnp.float32
BF16 = jnp.bfloat16
EPS = 1e-06
GATE_TEMP = 16.0
NY = 4
UNIT = 16


def dot(a, b):
    return jnp.dot(a, b, preferred_element_type=F32)


def dot_nt(a, b):
    return lax.dot_general(a, b, (((1,), (1,)), ((), ())), preferred_element_type=F32)


class Plan:
    def __init__(self, n_kv, n_tp, rows, feat, kd, vd, rank, hid, span):
        self.kv, self.tp, self.rows, self.feat = n_kv, n_tp, rows, feat
        self.kd, self.vd, self.rank, self.hid, self.span = kd, vd, rank, hid, span
        self.nz = n_kv // NY
        self.seqs = rows // n_kv
        self.width = feat * n_kv
        self.cols = 2 * kd + 2 * vd + 128
        units = -(-hid // (UNIT * NY))
        self.per_y = units * UNIT
        self.cnt = [UNIT * (units // self.nz + (1 if z < units % self.nz else 0)) for z in range(self.nz)]
        self.off = [sum(self.cnt[:z]) for z in range(self.nz)]
        self.pr = max(self.cnt)
        half = self.nz // 2
        step = max(1, half // 2)
        self.a_subs = [list(range(i, i + step)) for i in range(0, half, step)]
        self.b_subs = [list(range(i, i + step)) for i in range(half, self.nz, step)]
        self.subs = self.a_subs + self.b_subs
        self.na = len(self.a_subs)
        self.has_sq = [i in (0, self.na) for i in range(len(self.subs))]
        self.sub_rows = [
            (UNIT if sq else 0) + sum(2 * self.cnt[z] for z in zs)
            for sq, zs in zip(self.has_sq, self.subs)
        ]
        self.piece = UNIT + 2 * self.pr


def kernel(pn, *refs):
    it = iter(refs)
    take = lambda n: [next(it) for _ in range(n)]
    (
        tok_h, again_h, wq_h, wk_h, wv_h, wg_h, wc_h, dwt_h, bias_h, hgain_h,
        kc_h, vc_h, dc_h, st_h, len_h, ow_h, mgain_h, gw_h, uw_h, dn_h,
    ) = take(20)
    out_ref, nk_ref, nv_ref = take(3)
    (
        tok, again, wq, wk, wv, wg, wc, dwt, bias, hgain, kc, vc, dc, st, lens, ow, mgain, gw, uw, dn,
    ) = take(20)
    (f1, p1, r1, keyed, etot, stb, owt, tokt, mgt, dnp, dnt, g1, g1f, x1, midt, x2, spc, zin, hb) = take(19)
    ns = len(pn.subs)
    psub = take(ns)
    rin = take(ns)
    qin = take(ns)
    cin = take(ns)
    cout = take(ns)
    (
        in_sem, s1s, s1r, g1s, g1r, x1s, x1r, x2s, x2r,
        rss, rsr, qss, qsr, css, csr, zss, zsr, hzs, hzr, hls, hlr, hrs, hrr, hfs, hfr,
    ) = take(25)

    kv = lax.axis_index("kv")
    tp = lax.axis_index("tp")
    nz, n_kv, n_tp = pn.nz, pn.kv, pn.tp
    y = lax.rem(kv, NY)
    z = kv // NY
    yr, yl, yo = lax.rem(y + 1, NY), lax.rem(y + 3, NY), lax.rem(y + 2, NY)
    right, left = z * NY + yr, z * NY + yl

    pairs = [
        (tok_h, tok), (again_h, again), (wq_h, wq), (wk_h, wk), (wv_h, wv), (wg_h, wg),
        (wc_h, wc.at[pl.ds(0, pn.rank)]),
        (dc_h, dc), (len_h, lens), (kc_h, kc), (st_h, st), (dwt_h, dwt.at[pl.ds(0, pn.rank)]),
        (bias_h, bias), (hgain_h, hgain), (vc_h, vc), (ow_h, ow), (mgain_h, mgain),
    ]
    last = pn.hid - (NY - 1) * pn.per_y
    for src, dst in ((gw_h, gw), (uw_h, uw), (dn_h, dn)):
        for i in range(NY):
            size = pn.per_y if i < NY - 1 else last
            pairs.append((src.at[pl.ds(i * pn.per_y, size)], dst.at[i, pl.ds(0, size)]))
    wc[...] = jnp.zeros_like(wc)
    dwt[...] = jnp.zeros_like(dwt)
    loads = [pltpu.make_async_copy(s, d, in_sem.at[i]) for i, (s, d) in enumerate(pairs)]
    for c in loads:
        c.start()

    barrier = pltpu.get_barrier_semaphore()

    @pl.loop(1, n_kv)
    def _(d):
        pl.semaphore_signal(barrier, inc=1, device_id={"kv": lax.rem(kv + d, n_kv)}, device_id_type=MESH)

    @pl.loop(1, n_tp)
    def _(d):
        pl.semaphore_signal(barrier, inc=1, device_id={"tp": lax.rem(tp + d, n_tp)}, device_id_type=MESH)

    def remote(src, dst, ssem, rsem, **where):
        return pltpu.make_async_remote_copy(
            src_ref=src, dst_ref=dst, send_sem=ssem, recv_sem=rsem, device_id=where, device_id_type=MESH
        )

    def drain(ref, sem):
        pltpu.make_async_copy(ref, ref, sem).wait()

    for c in loads[:7]:
        c.wait()
    tok_f = tok[...].astype(F32)
    scaled = (tok_f * again[...]).astype(BF16)
    kd, vd = pn.kd, pn.vd
    f1[:, 0:kd] = dot(scaled, wq[...])
    f1[:, kd : 2 * kd] = dot(scaled, wk[...])
    f1[:, 2 * kd : 2 * kd + vd] = dot(scaled, wv[...])
    f1[:, 2 * kd + vd : 2 * kd + 2 * vd] = dot(scaled, wg[...])
    code = dot_nt(scaled, wc[...])
    squares = jnp.sum(tok_f * tok_f, axis=1, keepdims=True)
    lane = lax.broadcasted_iota(jnp.int32, code.shape, 1)
    f1[:, 2 * kd + 2 * vd :] = jnp.where(lane == pn.rank, squares, code)
    for p in range(n_kv):
        p1[p] = f1[p * pn.seqs : (p + 1) * pn.seqs, :].astype(BF16)
    pl.semaphore_wait(barrier, n_kv + n_tp - 2)

    @pl.loop(1, n_kv)
    def _(d):
        peer = lax.rem(kv + d, n_kv)
        remote(p1.at[peer], r1.at[kv], s1s, s1r, kv=peer).start()

    r1[kv] = p1[kv]

    for c in loads[7:17]:
        c.wait()
    pos = lax.broadcasted_iota(jnp.int32, (pn.span, kd), 0)
    for b in range(pn.seqs):
        live = pos < lens[b]
        kept = jnp.where(live, dc[b], 0.0)
        run = kept
        shift = 1
        while shift < pn.span:
            moved = pltpu.roll(run, pn.span - shift, 0)
            run = run + jnp.where(pos < pn.span - shift, moved, 0.0)
            shift *= 2
        keyed[b] = jnp.where(live, kc[b].astype(F32) * jnp.exp(run - kept), 0.0)
        etot[b : b + 1, :] = jnp.exp(run[0:1, :])
        stb[b] = st[b].astype(BF16)
    tokt[...] = tok_f.T
    mgt[...] = jnp.broadcast_to(mgain[...], (pn.rows, pn.feat)).T
    for i in range(vd // 128):
        owt[:, i * 128 : (i + 1) * 128] = ow[i * 128 : (i + 1) * 128, :].astype(F32).T.astype(BF16)
    for c in loads[17:]:
        c.wait()
    pad = NY * pn.per_y - pn.hid
    if pad:
        for ref in (gw, uw, dn):
            ref[NY - 1, pn.per_y - pad :, :] = jnp.zeros((pad, pn.feat), BF16)
    dnp[...] = jnp.zeros_like(dnp)
    spc[...] = jnp.zeros_like(spc)
    for i in range(NY):
        for zz in range(nz):
            dnp[i, zz * pn.pr : zz * pn.pr + pn.cnt[zz], :] = dn[i, pn.off[zz] : pn.off[zz] + pn.cnt[zz], :]
        for j in range(nz * pn.pr // 128):
            dnt[i, :, j * 128 : (j + 1) * 128] = (
                dnp[i, j * 128 : (j + 1) * 128, :].astype(F32).T.astype(BF16)
            )

    drain(r1.at[pl.ds(0, n_kv - 1)], s1r)
    sums = jnp.zeros((pn.seqs, pn.cols), F32)
    for p in range(n_kv):
        sums = sums + r1[p].astype(F32)
    tail = sums[:, 2 * kd + 2 * vd :]
    inv = lax.rsqrt(tail[:, pn.rank : pn.rank + 1] / pn.width + EPS)
    queries = (sums[:, 0:kd] * inv * kd ** (-0.5)).astype(BF16).astype(F32)
    new_keys = (sums[:, kd : 2 * kd] * inv).astype(BF16)
    new_values = (sums[:, 2 * kd : 2 * kd + vd] * inv).astype(BF16)
    out_gate = (sums[:, 2 * kd + vd : 2 * kd + 2 * vd] * inv).astype(BF16).astype(F32)
    nk_ref[...] = new_keys
    nv_ref[...] = new_values
    pre = dot((tail * inv).astype(BF16), dwt[...]) + bias[...]
    new_decay = (jnp.minimum(pre, 0.0) - jnp.log1p(jnp.exp(-jnp.abs(pre)))) / GATE_TEMP
    decayed = queries * jnp.exp(new_decay)
    faded = (decayed * etot[...]).astype(BF16)
    own = jnp.sum(queries * new_keys.astype(F32), axis=1, keepdims=True)
    rows = []
    for b in range(pn.seqs):
        scores = jnp.sum(decayed[b : b + 1, :] * keyed[b], axis=1, keepdims=True).astype(BF16).astype(F32)
        within = jnp.sum(scores * vc[b].astype(F32), axis=0, keepdims=True)
        rows.append(dot(faded, stb[b])[b : b + 1, :] + within)
    mixed = jnp.concatenate(rows, axis=0) + own * new_values.astype(F32)
    normed = mixed * lax.rsqrt(jnp.mean(mixed * mixed, axis=1, keepdims=True) + EPS) * hgain[...]
    heads = normed * (out_gate / (1.0 + jnp.exp(-out_gate)))
    g1[kv] = heads.astype(BF16)

    @pl.loop(1, n_kv)
    def _(d):
        peer = lax.rem(kv + d, n_kv)
        remote(g1.at[kv], g1.at[kv], g1s, g1r, kv=peer).start()

    drain(g1.at[pl.ds(0, n_kv - 1)], g1r)
    for p in range(n_kv):
        g1f[p * pn.seqs : (p + 1) * pn.seqs, :] = g1[p].astype(F32)

    def summed_over_tp(part, buf, ssem, rsem):
        buf[tp] = part.astype(BF16)

        @pl.loop(1, n_tp)
        def _(d):
            peer = lax.rem(tp + d, n_tp)
            remote(buf.at[tp], buf.at[tp], ssem, rsem, tp=peer).start()

        drain(buf.at[pl.ds(0, n_tp - 1)], rsem)
        total = buf[0].astype(F32)
        for i in range(1, n_tp):
            total = total + buf[i].astype(F32)
        return total

    attended = summed_over_tp(dot_nt(owt[...], g1f[...].astype(BF16)), x1, x1s, x1r)
    mid = (tokt[...] + attended).astype(BF16)
    mid_f = mid.astype(F32)
    midt[...] = mid_f
    scaled_mid = (mid_f * mgt[...]).astype(BF16)
    sq_rows = jnp.broadcast_to(jnp.sum(mid_f * mid_f, axis=0, keepdims=True), (UNIT, pn.rows)).astype(BF16)

    def fill(dest):
        gate = dot(gw[dest], scaled_mid).astype(BF16)
        up = dot(uw[dest], scaled_mid).astype(BF16)
        for s, zs in enumerate(pn.subs):
            at = 0
            if pn.has_sq[s]:
                psub[s][dest, 0:UNIT, :] = sq_rows
                at = UNIT
            for zz in zs:
                o, n = pn.off[zz], pn.cnt[zz]
                psub[s][dest, at : at + n, :] = gate[o : o + n, :]
                psub[s][dest, at + n : at + 2 * n, :] = up[o : o + n, :]
                at += 2 * n

    def toward(s):
        return right if s < pn.na else left

    def against(s):
        return left if s < pn.na else right

    fill(yo)
    for s in range(ns):
        remote(psub[s].at[yo], rin[s], rss.at[s], rsr.at[s], kv=toward(s)).start()
    fill(yr)
    for s in range(pn.na, ns):
        remote(psub[s].at[yr], qin[s], qss.at[s], qsr.at[s], kv=right).start()
    fill(yl)
    for s in range(pn.na):
        remote(psub[s].at[yl], qin[s], qss.at[s], qsr.at[s], kv=left).start()
    fill(y)
    order = []
    for i in range(max(pn.na, ns - pn.na)):
        order += [s for s in (i, pn.na + i) if (s < pn.na) == (s == i)]
    for s in order:
        nxt = yr if s < pn.na else yl
        drain(rin[s], rsr.at[s])
        cout[s][...] = (psub[s][nxt].astype(F32) + rin[s][...].astype(F32)).astype(BF16)
        remote(cout[s], cin[s], css.at[s], csr.at[s], kv=toward(s)).start()
    sq_sum = {}
    for s in order:
        drain(qin[s], qsr.at[s])
        drain(cin[s], csr.at[s])
        total = (psub[s][y].astype(F32) + qin[s][...].astype(F32) + cin[s][...].astype(F32)).astype(BF16)
        side = s < pn.na
        at = 0
        if pn.has_sq[s]:
            sq_sum[side] = total[0:UNIT, :]
            at = UNIT
        for zz in pn.subs[s]:
            n = pn.cnt[zz]
            spc[zz, 0:UNIT, :] = sq_sum[side]
            spc[zz, UNIT : UNIT + n, :] = total[at : at + n, :]
            spc[zz, UNIT + pn.pr : UNIT + pn.pr + n, :] = total[at + n : at + 2 * n, :]
            at += 2 * n

            @pl.when(z != zz)
            def _(zz=zz):
                remote(spc.at[zz], zin.at[z], zss, zsr, kv=zz * NY + y).start()

    zin[z] = spc[z]
    drain(zin.at[pl.ds(0, nz - 1)], zsr)
    total = zin[0].astype(F32)
    for i in range(1, nz):
        total = total + zin[i].astype(F32)
    inv_mid = lax.rsqrt(total[0:1, :] / pn.width + EPS)
    gate = total[UNIT : UNIT + pn.pr, :] * inv_mid
    up = total[UNIT + pn.pr :, :] * inv_mid
    hb[y, z] = (gate / (1.0 + jnp.exp(-gate)) * up).astype(BF16)

    for d in range(1, nz):
        remote(hb.at[y, z], hb.at[y, z], hzs.at[d], hzr.at[d], kv=lax.rem(z + d, nz) * NY + y).start()

    def slot(d):
        return lax.rem(z + nz - d, nz)

    def spread(d):
        if d:
            drain(hb.at[y, slot(d)], hzr.at[d])
        mine = hb.at[y, slot(d)]
        remote(mine, mine, hls.at[d], hlr.at[d], kv=right).start()
        remote(mine, mine, hrs.at[d], hrr.at[d], kv=left).start()

    def forward(d):
        drain(hb.at[yl, slot(d)], hlr.at[d])
        drain(hb.at[yr, slot(d)], hrr.at[d])
        if d % 2 == 0:
            other = hb.at[yl, slot(d)]
            remote(other, other, hfs.at[d], hfr.at[d], kv=right).start()
        else:
            other = hb.at[yr, slot(d)]
            remote(other, other, hfs.at[d], hfr.at[d], kv=left).start()

    near = sorted(range(nz), key=lambda d: min(d, nz - d))
    head, rest = near[:3], near[3:]
    for d in head:
        spread(d)
    forward(near[0])
    for d in rest:
        spread(d)
    for d in near[1:]:
        forward(d)

    def lifted_from(row):
        return dot(dnt[row], hb[row].reshape(nz * pn.pr, pn.rows))

    lifted = lifted_from(y) + lifted_from(yl) + lifted_from(yr)
    for d in near:
        drain(hb.at[yo, slot(d)], hfr.at[d])
    lifted = lifted + lifted_from(yo)
    final = midt[...] + summed_over_tp(lifted, x2, x2s, x2r)
    out_ref[...] = final.T.astype(BF16)

    drain(p1.at[pl.ds(0, n_kv - 1)], s1s)
    drain(g1.at[pl.ds(0, n_kv - 1)], g1s)
    drain(x1.at[pl.ds(0, n_tp - 1)], x1s)
    drain(x2.at[pl.ds(0, n_tp - 1)], x2s)
    for s in range(ns):
        drain(rin[s], rss.at[s])
        drain(qin[s], qss.at[s])
        drain(cin[s], css.at[s])
    drain(zin.at[pl.ds(0, nz - 1)], zss)
    for d in range(nz):
        if d:
            drain(hb.at[0, 0], hzs.at[d])
        drain(hb.at[0, 0], hls.at[d])
        drain(hb.at[0, 0], hrs.at[d])
        drain(hb.at[0, 0], hfs.at[d])


def on_device(n_kv, n_tp, *args):
    (
        tokens, attn_gain, query_weight, key_weight, value_weight, outgate_weight, code_weight,
        decay_weight, decay_bias, head_gain, key_cache, value_cache, decay_cache, carried_state,
        lengths, output_weight, mlp_gain, gate_weight, up_weight, down_weight,
    ) = args
    rows, feat = tokens.shape
    seqs, span, _, kd = key_cache.shape
    vd = value_cache.shape[-1]
    rank = code_weight.shape[1]
    hid = gate_weight.shape[1]
    pn = Plan(n_kv, n_tp, rows, feat, kd, vd, rank, hid, span)
    operands = (
        tokens, attn_gain.reshape(1, feat), query_weight, key_weight, value_weight, outgate_weight,
        code_weight.T, decay_weight, decay_bias.reshape(1, kd), head_gain.reshape(1, vd),
        key_cache.reshape(seqs, span, kd), value_cache.reshape(seqs, span, vd),
        decay_cache.reshape(seqs, span, kd), carried_state.reshape(seqs, kd, vd), lengths,
        output_weight, mlp_gain.reshape(1, feat), gate_weight.T, up_weight.T, down_weight,
    )
    nz, pr = pn.nz, pn.pr
    vm = pltpu.VMEM
    dma = pltpu.SemaphoreType.DMA
    ns = len(pn.subs)
    landing = [
        vm((rows, feat), BF16), vm((1, feat), F32), vm((feat, kd), BF16), vm((feat, kd), BF16),
        vm((feat, vd), BF16), vm((feat, vd), BF16), vm((128, feat), BF16), vm((128, kd), BF16),
        vm((1, kd), F32), vm((1, vd), F32), vm((seqs, span, kd), BF16), vm((seqs, span, vd), BF16),
        vm((seqs, span, kd), F32), vm((seqs, kd, vd), F32), pltpu.SMEM((seqs,), jnp.int32),
        vm((vd, feat), BF16), vm((1, feat), F32), vm((NY, pn.per_y, feat), BF16),
        vm((NY, pn.per_y, feat), BF16), vm((NY, pn.per_y, feat), BF16),
    ]
    work = [
        vm((rows, pn.cols), F32), vm((n_kv, seqs, pn.cols), BF16), vm((n_kv, seqs, pn.cols), BF16),
        vm((seqs, span, kd), F32), vm((seqs, kd), F32), vm((seqs, kd, vd), BF16),
        vm((feat, vd), BF16), vm((feat, rows), F32), vm((feat, rows), F32),
        vm((NY, nz * pr, feat), BF16), vm((NY, feat, nz * pr), BF16),
        vm((n_kv, seqs, vd), BF16), vm((rows, vd), F32), vm((n_tp, feat, rows), BF16),
        vm((feat, rows), F32), vm((n_tp, feat, rows), BF16),
        vm((nz, pn.piece, rows), BF16), vm((nz, pn.piece, rows), BF16), vm((NY, nz, pr, rows), BF16),
    ]
    subs = [vm((NY, n, rows), BF16) for n in pn.sub_rows]
    for _ in range(4):
        subs += [vm((n, rows), BF16) for n in pn.sub_rows]
    sems = [dma((17 + 3 * NY,))] + [dma(())] * 8 + [dma((ns,))] * 6 + [dma(())] * 2 + [dma((nz,))] * 8
    out, nk, nv = pl.pallas_call(
        functools.partial(kernel, pn),
        out_shape=(
            jax.ShapeDtypeStruct((rows, feat), BF16),
            jax.ShapeDtypeStruct((seqs, kd), BF16),
            jax.ShapeDtypeStruct((seqs, vd), BF16),
        ),
        in_specs=[pl.BlockSpec(memory_space=pl.ANY)] * len(operands),
        out_specs=(pl.BlockSpec(memory_space=pltpu.VMEM),) * 3,
        scratch_shapes=landing + work + subs + sems,
        compiler_params=pltpu.CompilerParams(
            collective_id=0, has_side_effects=True, vmem_limit_bytes=60 * 1024 * 1024
        ),
        name="decode_step",
    )(*operands)
    return out, nk.reshape(seqs, 1, kd), nv.reshape(seqs, 1, vd)


def solution(mesh):
    in_specs = (
        P(None, "kv"), P("kv"), P("kv", "tp"), P("kv", "tp"), P("kv", "tp"), P("kv", "tp"),
        P("kv", None), P(None, "tp"), P("tp"), P(), P("kv", None, "tp", None),
        P("kv", None, "tp", None), P("kv", None, "tp", None), P("kv", "tp", None, None), P("kv"),
        P("tp", "kv"), P("kv"), P("kv", "tp"), P("kv", "tp"), P("tp", "kv"),
    )
    out_specs = (P(None, "kv"), P("kv", "tp", None), P("kv", "tp", None))
    return jax.shard_map(
        functools.partial(on_device, mesh.shape["kv"], mesh.shape["tp"]),
        mesh=mesh, in_specs=in_specs, out_specs=out_specs, check_vma=False,
    )
```

```python
import functools

import jax
import jax.numpy as jnp
from jax import lax
from jax.experimental import pallas as pl
from jax.experimental.pallas import tpu as pltpu
from jax.sharding import PartitionSpec as P

MESH = pl.DeviceIdType.MESH
F32 = jnp.float32
BF16 = jnp.bfloat16
EPS = 1e-06
GATE_TEMP = 16.0
NY = 4
UNIT = 16


def dot(a, b):
    return jnp.dot(a, b, preferred_element_type=F32)


def dot_nt(a, b):
    return lax.dot_general(a, b, (((1,), (1,)), ((), ())), preferred_element_type=F32)


class Plan:
    def __init__(self, n_kv, n_tp, rows, feat, kd, vd, rank, hid, span):
        self.kv, self.tp, self.rows, self.feat = n_kv, n_tp, rows, feat
        self.kd, self.vd, self.rank, self.hid, self.span = kd, vd, rank, hid, span
        self.nz = n_kv // NY
        self.seqs = rows // n_kv
        self.width = feat * n_kv
        self.cols = 2 * kd + 2 * vd + 128
        units = -(-hid // (UNIT * NY))
        self.per_y = units * UNIT
        self.cnt = [UNIT * (units // self.nz + (1 if z < units % self.nz else 0)) for z in range(self.nz)]
        self.off = [sum(self.cnt[:z]) for z in range(self.nz)]
        self.pr = max(self.cnt)
        half = self.nz // 2
        step = max(1, half // 2)
        self.a_subs = [list(range(i, i + step)) for i in range(0, half, step)]
        self.b_subs = [list(range(i, i + step)) for i in range(half, self.nz, step)]
        self.subs = self.a_subs + self.b_subs
        self.na = len(self.a_subs)
        self.sub_rows = [sum(2 * self.cnt[z] for z in zs) for zs in self.subs]
        ring = lambda d, n: min(d, n - d)
        self.kv_far = sorted(
            [(dz, dy) for dz in range(self.nz) for dy in range(NY) if dz or dy],
            key=lambda o: -ring(o[0], self.nz) - ring(o[1], NY),
        )
        nx = n_tp // 2
        self.tp_far = sorted(
            [(dx, dc) for dx in range(nx) for dc in range(2) if dx or dc], key=lambda o: -2 * ring(o[0], nx) - o[1]
        )


def kernel(pn, *refs):
    it = iter(refs)
    take = lambda n: [next(it) for _ in range(n)]
    (
        tok_h, again_h, wq_h, wk_h, wv_h, wg_h, wc_h, dwt_h, bias_h, hgain_h,
        kc_h, vc_h, dc_h, st_h, len_h, ow_h, mgain_h, gw_h, uw_h, dn_h,
    ) = take(20)
    out_ref, nk_ref, nv_ref = take(3)
    (
        tok, again, wq, wk, wv, wg, wc, dwt, bias, hgain, kc, vc, dc, st, lens, ow, mgain, gw, uw, dn,
    ) = take(20)
    (f1, p1, r1, keyed, etot, stb, owt, tokt, mgt, dnp, dnt, g1, g1f, x1, midt, x2, spc, zin, hb, sqb) = take(20)
    ns = len(pn.subs)
    psub = take(ns)
    rin = take(ns)
    qin = take(ns)
    cin = take(ns)
    cout = take(ns)
    (
        in_sem, s1s, s1r, g1s, g1r, x1s, x1r, x2s, x2r,
        sqs, sqr, rss, rsr, qss, qsr, css, csr, zss, zsr, hzs, hzr, hls, hlr, hrs, hrr, hfs, hfr,
    ) = take(27)

    kv = lax.axis_index("kv")
    tp = lax.axis_index("tp")
    nz, n_kv, n_tp = pn.nz, pn.kv, pn.tp
    y = lax.rem(kv, NY)
    z = kv // NY
    yr, yl, yo = lax.rem(y + 1, NY), lax.rem(y + 3, NY), lax.rem(y + 2, NY)
    right, left, opposite = z * NY + yr, z * NY + yl, z * NY + yo

    def kv_peer(offset):
        return lax.rem(z + offset[0], nz) * NY + lax.rem(y + offset[1], NY)

    def tp_peer(offset):
        return lax.rem(tp // 2 + offset[0], n_tp // 2) * 2 + lax.rem(lax.rem(tp, 2) + offset[1], 2)

    barrier = pltpu.get_barrier_semaphore()
    for o in pn.kv_far:
        pl.semaphore_signal(barrier, inc=1, device_id={"kv": kv_peer(o)}, device_id_type=MESH)
    for o in pn.tp_far:
        pl.semaphore_signal(barrier, inc=1, device_id={"tp": tp_peer(o)}, device_id_type=MESH)

    pairs = [
        (tok_h, tok), (again_h, again), (wq_h, wq), (wk_h, wk), (wv_h, wv), (wg_h, wg),
        (wc_h, wc.at[pl.ds(0, pn.rank)]),
        (dc_h, dc), (len_h, lens), (kc_h, kc), (st_h, st), (dwt_h, dwt.at[pl.ds(0, pn.rank)]),
        (bias_h, bias), (hgain_h, hgain), (vc_h, vc), (ow_h, ow), (mgain_h, mgain),
    ]
    last = pn.hid - (NY - 1) * pn.per_y
    for src, dst in ((gw_h, gw), (uw_h, uw), (dn_h, dn)):
        for i in range(NY):
            size = pn.per_y if i < NY - 1 else last
            pairs.append((src.at[pl.ds(i * pn.per_y, size)], dst.at[i, pl.ds(0, size)]))
    wc[...] = jnp.zeros_like(wc)
    dwt[...] = jnp.zeros_like(dwt)
    loads = [pltpu.make_async_copy(s, d, in_sem.at[i]) for i, (s, d) in enumerate(pairs)]
    for c in loads:
        c.start()

    def remote(src, dst, ssem, rsem, **where):
        return pltpu.make_async_remote_copy(
            src_ref=src, dst_ref=dst, send_sem=ssem, recv_sem=rsem, device_id=where, device_id_type=MESH
        )

    def drain(ref, sem):
        pltpu.make_async_copy(ref, ref, sem).wait()

    pending = []

    for c in loads[:7]:
        c.wait()
    tok_f = tok[...].astype(F32)
    scaled = (tok_f * again[...]).astype(BF16)
    kd, vd = pn.kd, pn.vd
    f1[:, 0:kd] = dot(scaled, wq[...])
    f1[:, kd : 2 * kd] = dot(scaled, wk[...])
    f1[:, 2 * kd : 2 * kd + vd] = dot(scaled, wv[...])
    f1[:, 2 * kd + vd : 2 * kd + 2 * vd] = dot(scaled, wg[...])
    code = dot_nt(scaled, wc[...])
    squares = jnp.sum(tok_f * tok_f, axis=1, keepdims=True)
    lane = lax.broadcasted_iota(jnp.int32, code.shape, 1)
    f1[:, 2 * kd + 2 * vd :] = jnp.where(lane == pn.rank, squares, code)
    for p in range(n_kv):
        p1[p] = f1[p * pn.seqs : (p + 1) * pn.seqs, :].astype(BF16)
    pl.semaphore_wait(barrier, n_kv + n_tp - 2)

    for o in pn.kv_far:
        remote(p1.at[kv_peer(o)], r1.at[kv], s1s, s1r, kv=kv_peer(o)).start()

    pending.append((p1.at[pl.ds(0, n_kv - 1)], s1s))

    r1[kv] = p1[kv]

    for c in loads[7:17]:
        c.wait()
    pos = lax.broadcasted_iota(jnp.int32, (pn.span, kd), 0)
    for b in range(pn.seqs):
        live = pos < lens[b]
        kept = jnp.where(live, dc[b], 0.0)
        run = kept
        shift = 1
        while shift < pn.span:
            moved = pltpu.roll(run, pn.span - shift, 0)
            run = run + jnp.where(pos < pn.span - shift, moved, 0.0)
            shift *= 2
        keyed[b] = jnp.where(live, kc[b].astype(F32) * jnp.exp(run - kept), 0.0)
        etot[b : b + 1, :] = jnp.exp(run[0:1, :])
        stb[b] = st[b].astype(BF16)
    tokt[...] = tok_f.T
    mgt[...] = jnp.broadcast_to(mgain[...], (pn.rows, pn.feat)).T
    for i in range(vd // 128):
        owt[:, i * 128 : (i + 1) * 128] = ow[i * 128 : (i + 1) * 128, :].astype(F32).T.astype(BF16)
    for c in loads[17:]:
        c.wait()
    pad = NY * pn.per_y - pn.hid
    if pad:
        for ref in (gw, uw, dn):
            ref[NY - 1, pn.per_y - pad :, :] = jnp.zeros((pad, pn.feat), BF16)
    dnp[...] = jnp.zeros_like(dnp)
    spc[...] = jnp.zeros_like(spc)
    for i in range(NY):
        for zz in range(nz):
            dnp[i, zz * pn.pr : zz * pn.pr + pn.cnt[zz], :] = dn[i, pn.off[zz] : pn.off[zz] + pn.cnt[zz], :]
        for j in range(nz * pn.pr // 128):
            dnt[i, :, j * 128 : (j + 1) * 128] = (
                dnp[i, j * 128 : (j + 1) * 128, :].astype(F32).T.astype(BF16)
            )

    drain(r1.at[pl.ds(0, n_kv - 1)], s1r)
    sums = jnp.zeros((pn.seqs, pn.cols), F32)
    for p in range(n_kv):
        sums = sums + r1[p].astype(F32)
    tail = sums[:, 2 * kd + 2 * vd :]
    inv = lax.rsqrt(tail[:, pn.rank : pn.rank + 1] / pn.width + EPS)
    queries = (sums[:, 0:kd] * inv * kd ** (-0.5)).astype(BF16).astype(F32)
    new_keys = (sums[:, kd : 2 * kd] * inv).astype(BF16)
    new_values = (sums[:, 2 * kd : 2 * kd + vd] * inv).astype(BF16)
    out_gate = (sums[:, 2 * kd + vd : 2 * kd + 2 * vd] * inv).astype(BF16).astype(F32)
    nk_ref[...] = new_keys
    nv_ref[...] = new_values
    pre = dot((tail * inv).astype(BF16), dwt[...]) + bias[...]
    new_decay = (jnp.minimum(pre, 0.0) - jnp.log1p(jnp.exp(-jnp.abs(pre)))) / GATE_TEMP
    decayed = queries * jnp.exp(new_decay)
    faded = (decayed * etot[...]).astype(BF16)
    own = jnp.sum(queries * new_keys.astype(F32), axis=1, keepdims=True)
    rows = []
    for b in range(pn.seqs):
        scores = jnp.sum(decayed[b : b + 1, :] * keyed[b], axis=1, keepdims=True).astype(BF16).astype(F32)
        within = jnp.sum(scores * vc[b].astype(F32), axis=0, keepdims=True)
        rows.append(dot(faded, stb[b])[b : b + 1, :] + within)
    mixed = jnp.concatenate(rows, axis=0) + own * new_values.astype(F32)
    normed = mixed * lax.rsqrt(jnp.mean(mixed * mixed, axis=1, keepdims=True) + EPS) * hgain[...]
    heads = normed * (out_gate / (1.0 + jnp.exp(-out_gate)))
    g1[kv] = heads.astype(BF16)

    for o in pn.kv_far:
        remote(g1.at[kv], g1.at[kv], g1s, g1r, kv=kv_peer(o)).start()

    pending.append((g1.at[pl.ds(0, n_kv - 1)], g1s))

    drain(g1.at[pl.ds(0, n_kv - 1)], g1r)
    for p in range(n_kv):
        g1f[p * pn.seqs : (p + 1) * pn.seqs, :] = g1[p].astype(F32)

    def summed_over_tp(part, buf, ssem, rsem):
        buf[tp] = part.astype(BF16)

        for o in pn.tp_far:
            remote(buf.at[tp], buf.at[tp], ssem, rsem, tp=tp_peer(o)).start()

        pending.append((buf.at[pl.ds(0, n_tp - 1)], ssem))

        drain(buf.at[pl.ds(0, n_tp - 1)], rsem)
        total = buf[0].astype(F32)
        for i in range(1, n_tp):
            total = total + buf[i].astype(F32)
        return total

    attended = summed_over_tp(dot_nt(owt[...], g1f[...].astype(BF16)), x1, x1s, x1r)
    mid = (tokt[...] + attended).astype(BF16)
    mid_f = mid.astype(F32)
    midt[...] = mid_f
    scaled_mid = (mid_f * mgt[...]).astype(BF16)
    sqb[kv] = jnp.sum(mid_f * mid_f, axis=0, keepdims=True)

    def fill(dest):
        gate = dot(gw[dest], scaled_mid).astype(BF16)
        up = dot(uw[dest], scaled_mid).astype(BF16)
        for s, zs in enumerate(pn.subs):
            at = 0
            for zz in zs:
                o, n = pn.off[zz], pn.cnt[zz]
                psub[s][dest, at : at + n, :] = gate[o : o + n, :]
                psub[s][dest, at + n : at + 2 * n, :] = up[o : o + n, :]
                at += 2 * n

    def toward(s):
        return right if s < pn.na else left

    def against(s):
        return left if s < pn.na else right

    fill(yo)
    for s in range(ns):
        remote(psub[s].at[yo], rin[s], rss.at[s], rsr.at[s], kv=toward(s)).start()
        pending.append((rin[s], rss.at[s]))
    fill(yr)
    for s in range(pn.na, ns):
        remote(psub[s].at[yr], qin[s], qss.at[s], qsr.at[s], kv=right).start()
        pending.append((qin[s], qss.at[s]))
    fill(yl)
    for s in range(pn.na):
        remote(psub[s].at[yl], qin[s], qss.at[s], qsr.at[s], kv=left).start()
        pending.append((qin[s], qss.at[s]))
    fill(y)
    for o in pn.kv_far:
        remote(sqb.at[kv], sqb.at[kv], sqs, sqr, kv=kv_peer(o)).start()
    pending.append((sqb.at[pl.ds(0, n_kv - 1)], sqs))
    order = []
    for i in range(max(pn.na, ns - pn.na)):
        order += [s for s in (i, pn.na + i) if (s < pn.na) == (s == i)]
    for s in order:
        nxt = yr if s < pn.na else yl
        drain(rin[s], rsr.at[s])
        cout[s][...] = (psub[s][nxt].astype(F32) + rin[s][...].astype(F32)).astype(BF16)
        remote(cout[s], cin[s], css.at[s], csr.at[s], kv=toward(s)).start()
        pending.append((cin[s], css.at[s]))
    for s in order:
        drain(qin[s], qsr.at[s])
        drain(cin[s], csr.at[s])
        total = (psub[s][y].astype(F32) + qin[s][...].astype(F32) + cin[s][...].astype(F32)).astype(BF16)
        at = 0
        for zz in pn.subs[s]:
            n = pn.cnt[zz]
            spc[zz, 0:n, :] = total[at : at + n, :]
            spc[zz, pn.pr : pn.pr + n, :] = total[at + n : at + 2 * n, :]
            at += 2 * n

            @pl.when(z != zz)
            def _(zz=zz):
                remote(spc.at[zz], zin.at[z], zss, zsr, kv=zz * NY + y).start()

    pending.append((zin.at[pl.ds(0, nz - 1)], zss))
    zin[z] = spc[z]
    drain(zin.at[pl.ds(0, nz - 1)], zsr)
    total = zin[0].astype(F32)
    for i in range(1, nz):
        total = total + zin[i].astype(F32)
    drain(sqb.at[pl.ds(0, n_kv - 1)], sqr)
    inv_mid = lax.rsqrt(jnp.sum(sqb[...], axis=0) / pn.width + EPS)
    gate = total[0 : pn.pr, :] * inv_mid
    up = total[pn.pr :, :] * inv_mid
    hb[y, z] = (gate / (1.0 + jnp.exp(-gate)) * up).astype(BF16)

    for d in sorted(range(1, nz), key=lambda d: -min(d, nz - d)):
        remote(hb.at[y, z], hb.at[y, z], hzs.at[d], hzr.at[d], kv=lax.rem(z + d, nz) * NY + y).start()
        pending.append((hb.at[0, 0], hzs.at[d]))

    def slot(d):
        return lax.rem(z + nz - d, nz)

    def spread(d):
        if d:
            drain(hb.at[y, slot(d)], hzr.at[d])
        mine = hb.at[y, slot(d)]
        remote(mine, mine, hfs.at[d], hfr.at[d], kv=opposite).start()
        remote(mine, mine, hls.at[d], hlr.at[d], kv=right).start()
        remote(mine, mine, hrs.at[d], hrr.at[d], kv=left).start()
        pending.append((hb.at[0, 0], hfs.at[d]))
        pending.append((hb.at[0, 0], hls.at[d]))
        pending.append((hb.at[0, 0], hrs.at[d]))

    near = sorted(range(nz), key=lambda d: min(d, nz - d))
    for d in near:
        spread(d)

    def lifted_from(row):
        return dot(dnt[row], hb[row].reshape(nz * pn.pr, pn.rows))

    lifted = lifted_from(y)
    for d in near:
        drain(hb.at[yl, slot(d)], hlr.at[d])
        drain(hb.at[yr, slot(d)], hrr.at[d])
    lifted = lifted + lifted_from(yl) + lifted_from(yr)
    for d in near:
        drain(hb.at[yo, slot(d)], hfr.at[d])
    lifted = lifted + lifted_from(yo)
    final = midt[...] + summed_over_tp(lifted, x2, x2s, x2r)
    out_ref[...] = final.T.astype(BF16)

    for ref, sem in pending:
        drain(ref, sem)


def hand_over(a, b, c, ao, bo, co):
    ao[...] = a[...]
    bo[...] = b[...]
    co[...] = c[...]


def on_device(n_kv, n_tp, *args):
    (
        tokens, attn_gain, query_weight, key_weight, value_weight, outgate_weight, code_weight,
        decay_weight, decay_bias, head_gain, key_cache, value_cache, decay_cache, carried_state,
        lengths, output_weight, mlp_gain, gate_weight, up_weight, down_weight,
    ) = args
    rows, feat = tokens.shape
    seqs, span, _, kd = key_cache.shape
    vd = value_cache.shape[-1]
    rank = code_weight.shape[1]
    hid = gate_weight.shape[1]
    pn = Plan(n_kv, n_tp, rows, feat, kd, vd, rank, hid, span)
    operands = (
        tokens, attn_gain.reshape(1, feat), query_weight, key_weight, value_weight, outgate_weight,
        code_weight.T, decay_weight, decay_bias.reshape(1, kd), head_gain.reshape(1, vd),
        key_cache.reshape(seqs, span, kd), value_cache.reshape(seqs, span, vd),
        decay_cache.reshape(seqs, span, kd), carried_state.reshape(seqs, kd, vd), lengths,
        output_weight, mlp_gain.reshape(1, feat), gate_weight.T, up_weight.T, down_weight,
    )
    nz, pr = pn.nz, pn.pr
    vm = pltpu.VMEM
    dma = pltpu.SemaphoreType.DMA
    ns = len(pn.subs)
    landing = [
        vm((rows, feat), BF16), vm((1, feat), F32), vm((feat, kd), BF16), vm((feat, kd), BF16),
        vm((feat, vd), BF16), vm((feat, vd), BF16), vm((128, feat), BF16), vm((128, kd), BF16),
        vm((1, kd), F32), vm((1, vd), F32), vm((seqs, span, kd), BF16), vm((seqs, span, vd), BF16),
        vm((seqs, span, kd), F32), vm((seqs, kd, vd), F32), pltpu.SMEM((seqs,), jnp.int32),
        vm((vd, feat), BF16), vm((1, feat), F32), vm((NY, pn.per_y, feat), BF16),
        vm((NY, pn.per_y, feat), BF16), vm((NY, pn.per_y, feat), BF16),
    ]
    work = [
        vm((rows, pn.cols), F32), vm((n_kv, seqs, pn.cols), BF16), vm((n_kv, seqs, pn.cols), BF16),
        vm((seqs, span, kd), F32), vm((seqs, kd), F32), vm((seqs, kd, vd), BF16),
        vm((feat, vd), BF16), vm((feat, rows), F32), vm((feat, rows), F32),
        vm((NY, nz * pr, feat), BF16), vm((NY, feat, nz * pr), BF16),
        vm((n_kv, seqs, vd), BF16), vm((rows, vd), F32), vm((n_tp, feat, rows), BF16),
        vm((feat, rows), F32), vm((n_tp, feat, rows), BF16),
        vm((nz, 2 * pn.pr, rows), BF16), vm((nz, 2 * pn.pr, rows), BF16), vm((NY, nz, pr, rows), BF16),
        vm((n_kv, 1, rows), F32),
    ]
    subs = [vm((NY, n, rows), BF16) for n in pn.sub_rows]
    for _ in range(4):
        subs += [vm((n, rows), BF16) for n in pn.sub_rows]
    sems = [dma((17 + 3 * NY,))] + [dma(())] * 10 + [dma((ns,))] * 6 + [dma(())] * 2 + [dma((nz,))] * 8
    out, nk, nv = pl.pallas_call(
        functools.partial(kernel, pn),
        out_shape=(
            jax.ShapeDtypeStruct((rows, feat), BF16),
            jax.ShapeDtypeStruct((seqs, kd), BF16),
            jax.ShapeDtypeStruct((seqs, vd), BF16),
        ),
        in_specs=[pl.BlockSpec(memory_space=pl.ANY)] * len(operands),
        out_specs=(pl.BlockSpec(memory_space=pltpu.VMEM),) * 3,
        scratch_shapes=landing + work + subs + sems,
        compiler_params=pltpu.CompilerParams(
            collective_id=0, has_side_effects=True, vmem_limit_bytes=60 * 1024 * 1024
        ),
        name="decode_step",
    )(*operands)
    out, nk, nv = pl.pallas_call(
        hand_over,
        out_shape=(
            jax.ShapeDtypeStruct((rows, feat), BF16),
            jax.ShapeDtypeStruct((seqs, kd), BF16),
            jax.ShapeDtypeStruct((seqs, vd), BF16),
        ),
        in_specs=[pl.BlockSpec(memory_space=pltpu.VMEM)] * 3,
        out_specs=(pl.BlockSpec(memory_space=pltpu.VMEM),) * 3,
        name="hand_over",
    )(out, nk, nv)
    return out, nk.reshape(seqs, 1, kd), nv.reshape(seqs, 1, vd)


def solution(mesh):
    in_specs = (
        P(None, "kv"), P("kv"), P("kv", "tp"), P("kv", "tp"), P("kv", "tp"), P("kv", "tp"),
        P("kv", None), P(None, "tp"), P("tp"), P(), P("kv", None, "tp", None),
        P("kv", None, "tp", None), P("kv", None, "tp", None), P("kv", "tp", None, None), P("kv"),
        P("tp", "kv"), P("kv"), P("kv", "tp"), P("kv", "tp"), P("tp", "kv"),
    )
    out_specs = (P(None, "kv"), P("kv", "tp", None), P("kv", "tp", None))
    return jax.shard_map(
        functools.partial(on_device, mesh.shape["kv"], mesh.shape["tp"]),
        mesh=mesh, in_specs=in_specs, out_specs=out_specs, check_vma=False,
    )
```
